32 devices in a mesh: sp: 4 (over z), fs: 4 (over y, x), tp: 2 (over core).
Axes of the slice: x: 2, y: 2, z: 4, core: 2. Of those that a mesh axis runs over, the one named last changes fastest.
Arguments:
- tokens: bfloat16 [4, 2048, 2048], P('fs', 'sp', 'tp'), may hold values from -6 to 6
- norm_gain: float32 [2048], replicated, may hold values from 0.1 to 1.9
- w_pool_in: bfloat16 [2048, 512], P('fs', 'tp'), may hold values from -0.125 to 0.125
- w_query: bfloat16 [2048, 1024], P('fs', 'tp'), may hold values from -0.125 to 0.125
- w_key: bfloat16 [2048, 1024], P('fs', 'tp'), may hold values from -0.125 to 0.125
- w_value: bfloat16 [2048, 1024], P('fs', 'tp'), may hold values from -0.125 to 0.125
- query_gain: float32 [64], replicated, may hold values from 1.5 to 2.5
- key_gain: float32 [64], replicated, may hold values from 1.5 to 2.5
- stick_offset: float32 [16], P('tp'), as said below
- pool_mix: bfloat16 [4, 128, 128], P('tp'), may hold values from -0.5 to 0.5
- pool_scale: float32 [512], P('tp'), may hold values from 0.2 to 4, as said below
- pool_gain: bfloat16 [512], P('tp'), may hold values from 0.099609375 to 1.8984375
- attn_gain: bfloat16 [1024], P('tp'), may hold values from 0.099609375 to 1.8984375
- w_out_pool: bfloat16 [512, 2048], P('tp', 'fs'), may hold values from -0.15625 to 0.15625
- w_out_attn: bfloat16 [1024, 2048], P('tp', 'fs'), may hold values from -0.15625 to 0.15625
Outputs:
- mixed: bfloat16 [4, 2048, 2048], P('fs', ('sp', 'tp'))
The draws below stay inside these ranges and needn't reach their ends.
Inputs may be any that keep to these rules, and one draw needn't show every extreme that they name: `stick_offset`: per head, negative. `pool_scale`: positive channel scales.
All inputs are finite; a program needn't handle non-finite values.
Results may differ from the reference program's by a relative error of at most 0.013.
Values may be sent and summed in bfloat16 or wider, within the bound.
A program may use at most 192 MiB of HBM per device.

```python
import math
import jax
import jax.numpy as jnp
from jax import lax

D = 2048
HEADS = 16
HEAD_DIM = 64
POOL = 512
POOL_GROUPS = 4
TOK_DEV = 512
ATTN = 1024
LEN = 2048
SEQS = 4


def draw_stick_offset(key, part):
    key_fast = jax.random.fold_in(key, 11)
    key_slow = jax.random.fold_in(key, 12)
    key_quick = jax.random.fold_in(key, 13)
    chosen = jax.random.bernoulli(key_fast, 0.5, (HEADS,))
    slow_value = -(math.log(LEN) + jax.random.uniform(key_slow, (HEADS,), jnp.float32, 4.5, 5.5))
    fast_value = jax.random.uniform(key_quick, (HEADS,), jnp.float32, -8.5, -7.0)
    return jnp.where(chosen, fast_value, slow_value).astype(jnp.float32)


def draw_pool_scale(key, part):
    key_group = jax.random.fold_in(key, 21)
    key_channel = jax.random.fold_in(key, 22)
    group_factor = jnp.exp(jax.random.uniform(key_group, (POOL_GROUPS,), jnp.float32, math.log(0.3), math.log(3.0)))
    channel_factor = 1.0 + 0.18 * jax.random.uniform(key_channel, (POOL_GROUPS, POOL // POOL_GROUPS), jnp.float32, -1.0, 1.0)
    return (group_factor[:, None] * channel_factor).reshape(POOL).astype(jnp.float32)


def shard_levels(stream_key, shape, cuts, low, top_value):
    loudness = 1.0
    for axis_at, parts in cuts:
        heights = jax.random.uniform(jax.random.fold_in(jax.random.fold_in(stream_key, 6), axis_at), (parts,), jnp.float32, low / len(cuts), top_value / len(cuts))
        loudness = loudness * jnp.repeat(jnp.exp(heights), shape[axis_at] // parts).reshape((-1,) + (1,) * (len(shape) - 1 - axis_at))
    return loudness


def noise(rng, dims, width, bound, cuts=(), held_as=jnp.bfloat16):
    level = shard_levels(rng, dims, cuts, -0.22, 0.18) if cuts else 1.0
    values = jax.random.normal(rng, dims, jnp.float32) * width * level
    return jnp.minimum(jnp.maximum(values, -bound), bound).astype(held_as)


def setup_inputs(seed: int = 0) -> dict:
    streams_of = jax.random.split(jax.random.key(seed), 16)
    return {
        "tokens": noise(streams_of[0], (SEQS, LEN, D), 1.0, 6.0, ((0, 4), (1, 4), (2, 2))),
        "norm_gain": jnp.clip(1.0 + 0.18 * jax.random.normal(streams_of[1], (D,), jnp.float32), 0.1, 1.9),
        "w_pool_in": noise(streams_of[2], (D, POOL), D ** -0.5, 0.125, ((0, 4), (1, 2))),
        "w_query": noise(streams_of[3], (D, ATTN), D ** -0.5, 0.125, ((0, 4), (1, 2))),
        "w_key": noise(streams_of[4], (D, ATTN), D ** -0.5, 0.125, ((0, 4), (1, 2))),
        "w_value": noise(streams_of[5], (D, ATTN), D ** -0.5, 0.125, ((0, 4), (1, 2))),
        "query_gain": jnp.clip(jax.random.uniform(streams_of[6], (HEAD_DIM,), jnp.float32, 1.5, 2.5), 1.5, 2.5),
        "key_gain": jnp.clip(jax.random.uniform(streams_of[7], (HEAD_DIM,), jnp.float32, 1.5, 2.5), 1.5, 2.5),
        "stick_offset": draw_stick_offset(jax.random.fold_in(streams_of[15], 71), 0),
        "pool_mix": noise(streams_of[9], (POOL_GROUPS, POOL // POOL_GROUPS, POOL // POOL_GROUPS), (POOL // POOL_GROUPS) ** -0.5, 0.5, ((0, 2),)),
        "pool_scale": draw_pool_scale(jax.random.fold_in(streams_of[15], 71), 0),
        "pool_gain": jnp.clip(1.0 + 0.18 * jax.random.normal(streams_of[11], (POOL,), jnp.float32), 0.099609375, 1.8984375).astype(jnp.bfloat16),
        "attn_gain": jnp.clip(1.0 + 0.18 * jax.random.normal(streams_of[12], (ATTN,), jnp.float32), 0.099609375, 1.8984375).astype(jnp.bfloat16),
        "w_out_pool": noise(streams_of[13], (POOL, D), (POOL + ATTN) ** -0.5, 0.15625, ((0, 2), (1, 4))),
        "w_out_attn": noise(streams_of[14], (ATTN, D), (POOL + ATTN) ** -0.5, 0.15625, ((0, 2), (1, 4))),
    }


EPS = 1e-06
windows = (2, 4, 8, 16)

def row_norm(values_in, gain):
    values_f = values_in.astype(jnp.float32)
    factor = lax.rsqrt(lax.optimization_barrier(jnp.mean(values_f * values_f, axis=-1, keepdims=True)) + EPS)
    return (values_f * factor * gain.astype(jnp.float32)).astype(jnp.bfloat16)

def pool_branch(pool_in, pool_mix, pool_scale):
    group_ch = POOL // POOL_GROUPS
    values_f = pool_in.astype(jnp.float32).reshape(LEN, POOL_GROUPS, group_ch)
    position = jnp.arange(LEN, dtype=jnp.int32)
    pieces = []
    for group, window in enumerate(windows):
        column = values_f[:, group]
        padded = jnp.pad(column, ((window, 0), (0, 0)))
        summed = padded[window:window + LEN]
        for behind in range(1, window):
            summed = summed + padded[window - behind:window - behind + LEN]
        counted = jnp.minimum(position + 1, window).astype(jnp.float32)[:, None]
        pieces.append(summed / counted - column)
    centered = jnp.stack(pieces, axis=1).astype(jnp.bfloat16)
    pooled = jnp.einsum('sgc,gcd->sgd', centered.astype(jnp.float32), pool_mix.astype(jnp.float32))
    return (pooled.reshape(LEN, POOL) * pool_scale).astype(jnp.bfloat16)

def stick_branch(query, key_heads, value_heads, stick_offset):
    block_rows = TOK_DEV
    blocks = LEN // block_rows
    score_scale = 1.0 / math.sqrt(HEAD_DIM)
    query_h = query.transpose(1, 0, 2).reshape(HEADS, blocks, block_rows, HEAD_DIM)
    key_h = key_heads.transpose(1, 0, 2)
    value_h = value_heads.transpose(1, 0, 2)
    key_pos = jnp.arange(LEN, dtype=jnp.int32)

    def per_head(head_args):
        query_blocks, key_one, value_one, offset = head_args

        def per_block(block_args):
            query_block, block_index = block_args
            scores = jnp.dot(query_block, key_one.T, preferred_element_type=jnp.float32) * score_scale + offset
            query_pos = block_index * block_rows + jnp.arange(block_rows, dtype=jnp.int32)
            causal = key_pos[None, :] < query_pos[:, None]
            keep = jnp.where(causal, jax.nn.log_sigmoid(-scores), 0.0)
            running = jnp.cumsum(keep, axis=-1)
            log_weight = jax.nn.log_sigmoid(scores) + running[:, -1:] - running
            weight = jnp.where(causal, jnp.exp(log_weight), 0.0).astype(jnp.bfloat16)
            return jnp.dot(weight, value_one, preferred_element_type=jnp.float32)
        return lax.map(per_block, (query_blocks, jnp.arange(blocks, dtype=jnp.int32)))
    result = lax.map(per_head, (query_h, key_h, value_h, stick_offset))
    result = result.reshape(HEADS, LEN, HEAD_DIM).transpose(1, 0, 2)
    return result.reshape(LEN, ATTN).astype(jnp.bfloat16)

def head_norm(projected, gain):
    split = projected.reshape(LEN, HEADS, HEAD_DIM)
    factor = lax.rsqrt(lax.optimization_barrier(jnp.mean(split * split, axis=-1, keepdims=True)) + EPS)
    return (split * factor * gain).astype(jnp.bfloat16)

def one_sequence(tokens, norm_gain, w_pool_in, w_query, w_key, w_value, query_gain, key_gain, stick_offset, pool_mix, pool_scale, pool_gain, attn_gain, w_out_pool, w_out_attn):
    normed = row_norm(tokens, norm_gain)
    pool_in = jnp.dot(normed, w_pool_in, preferred_element_type=jnp.float32).astype(jnp.bfloat16)
    query = head_norm(jnp.dot(normed, w_query, preferred_element_type=jnp.float32), query_gain)
    key_heads = head_norm(jnp.dot(normed, w_key, preferred_element_type=jnp.float32), key_gain)
    value_heads = jnp.dot(normed, w_value, preferred_element_type=jnp.float32).astype(jnp.bfloat16).reshape(LEN, HEADS, HEAD_DIM)
    pooled = pool_branch(pool_in, pool_mix, pool_scale)
    attended = stick_branch(query, key_heads, value_heads, stick_offset)
    pool_normed = row_norm(pooled, pool_gain)
    attn_normed = row_norm(attended, attn_gain)
    summed = jnp.dot(pool_normed, w_out_pool, preferred_element_type=jnp.float32) + jnp.dot(attn_normed, w_out_attn, preferred_element_type=jnp.float32)
    return summed.astype(jnp.bfloat16)

def reference(tokens, norm_gain, w_pool_in, w_query, w_key, w_value, query_gain, key_gain, stick_offset, pool_mix, pool_scale, pool_gain, attn_gain, w_out_pool, w_out_attn):
    results = []
    for sequence in range(SEQS):
        results.append(one_sequence(tokens[sequence], norm_gain, w_pool_in, w_query, w_key, w_value, query_gain, key_gain, stick_offset, pool_mix, pool_scale, pool_gain, attn_gain, w_out_pool, w_out_attn))
    return jnp.stack(results)
```

```python
import math

import jax
import jax.numpy as jnp
from jax import lax
from jax.experimental import pallas as pl
from jax.experimental.pallas import tpu as pltpu
from jax.sharding import PartitionSpec as P

HEADS = 16
HEAD_DIM = 64
POOL = 512
POOL_GROUPS = 4


EPS = 1e-06


def shifted_2(value, axis, steps):
    count = lax.axis_size(axis)
    initial, last = (max(0, -steps), min(count, count - steps))
    return lax.ppermute(value, axis, [(source, source + steps) for source in range(initial, last)])


def head_norm(projected, gain, head_count):
    split = projected.reshape(projected.shape[0], head_count, HEAD_DIM)
    factor = lax.rsqrt(jnp.mean(split * split, axis=-1, keepdims=True) + EPS)
    return (split * factor * gain).astype(jnp.bfloat16)


def stick_block(query, key_heads, value_heads, offset, carried, row_offset, score_scale):
    scores = (
        jnp.einsum("thd,khd->htk", query, key_heads, preferred_element_type=jnp.float32)
        * score_scale
        + offset[:, None, None]
    )
    keep = jax.nn.log_sigmoid(-scores)
    if row_offset is not None:
        shape = (query.shape[0], key_heads.shape[0])
        earlier = (
            lax.broadcasted_iota(jnp.int32, shape, 1)
            < lax.broadcasted_iota(jnp.int32, shape, 0) + row_offset
        )
        keep = jnp.where(earlier[None], keep, 0.0)
    running = jnp.cumsum(keep, axis=2)
    block_total = running[:, :, -1]
    log_weight = (
        jax.nn.log_sigmoid(scores) + block_total[:, :, None] - running + carried[:, :, None]
    )
    weight = jnp.exp(log_weight)
    if row_offset is not None:
        weight = jnp.where(earlier[None], weight, 0.0)
    weight = weight.astype(jnp.bfloat16)
    block_out = jnp.einsum("htk,khd->thd", weight, value_heads, preferred_element_type=jnp.float32)
    return (block_out, block_total)


def branch_norm(values_in, squares, width, gain):
    values_f = values_in.astype(jnp.float32)
    factor = lax.rsqrt(squares / width + EPS)
    return (values_f * factor[:, None] * gain.astype(jnp.float32)).astype(jnp.bfloat16)


def shards(
    tokens,
    norm_gain,
    w_pool_in,
    w_query,
    w_key,
    w_value,
    query_gain,
    key_gain,
    stick_offset,
    pool_mix,
    pool_scale,
    pool_gain,
    attn_gain,
    w_out_pool,
    w_out_attn,
):
    whole = lax.all_gather(tokens, "tp", axis=2, tiled=True)[0]
    whole_f = whole.astype(jnp.float32)
    normed = (
        whole_f * lax.rsqrt(jnp.mean(whole_f * whole_f, axis=-1, keepdims=True) + EPS) * norm_gain
    ).astype(jnp.bfloat16)
    row_count = normed.shape[0]
    pieces = (
        lax.all_gather(w_pool_in, "fs", axis=0, tiled=True),
        lax.all_gather(w_query, "fs", axis=0, tiled=True),
        lax.all_gather(w_key, "fs", axis=0, tiled=True),
        lax.all_gather(w_value, "fs", axis=0, tiled=True),
    )
    pool_raw, query_raw, key_raw, value_raw = tuple(
        (jnp.dot(normed, piece, preferred_element_type=jnp.float32) for piece in pieces)
    )
    head_count = query_raw.shape[1] // HEAD_DIM
    query = head_norm(query_raw, query_gain, head_count)
    key_heads = head_norm(key_raw, key_gain, head_count)
    value_heads = value_raw.astype(jnp.bfloat16).reshape(row_count, head_count, HEAD_DIM)
    reach = 16
    pool_in = pool_raw.astype(jnp.bfloat16)
    previous = shifted_2(pool_in[row_count - reach :], "sp", 1)
    extended = jnp.concatenate([previous, pool_in], axis=0).astype(jnp.float32)
    pool_cols = pool_in.shape[1]
    group_ch = POOL // POOL_GROUPS
    local_groups = pool_cols // group_ch
    group_ids = (
        lax.axis_index("tp") * local_groups + jnp.arange(pool_cols, dtype=jnp.int32) // group_ch
    )
    window = jnp.left_shift(jnp.int32(2), group_ids)
    summed = jnp.zeros((row_count, pool_cols), jnp.float32)
    for behind in range(reach):
        shifted = extended[reach - behind : reach - behind + row_count]
        summed = summed + jnp.where(behind < window[None, :], shifted, 0.0)
    sp_index = lax.axis_index("sp")
    position = sp_index * row_count + jnp.arange(row_count, dtype=jnp.int32)
    counted = jnp.minimum(position[:, None] + 1, window[None, :]).astype(jnp.float32)
    centered = (summed / counted - extended[reach:]).astype(jnp.bfloat16)
    pooled = jnp.einsum(
        "tgc,gcd->tgd",
        centered.reshape(row_count, local_groups, group_ch),
        pool_mix,
        preferred_element_type=jnp.float32,
    )
    pool_out = (pooled.reshape(row_count, pool_cols) * pool_scale).astype(jnp.bfloat16)
    score_scale = 1.0 / math.sqrt(HEAD_DIM)
    sp_count = lax.axis_size("sp")
    key_value = jnp.stack([key_heads, value_heads])
    start_carry = jnp.zeros((head_count, row_count), jnp.float32)
    output, carried = stick_block(
        query, key_heads, value_heads, stick_offset, start_carry, 0, score_scale
    )
    everything = lax.all_gather(key_value, "sp", axis=1, tiled=True)

    def turn(turn_index, state):
        acc_out, acc_carry = state
        source = jnp.maximum(sp_index - turn_index, 0)
        block = lax.dynamic_slice_in_dim(everything, source * row_count, row_count, 1)
        block_out, block_total = stick_block(
            query, block[0], block[1], stick_offset, acc_carry, None, score_scale
        )
        usable = turn_index <= sp_index
        return (
            acc_out + jnp.where(usable, block_out, 0.0),
            acc_carry + jnp.where(usable, block_total, 0.0),
        )

    output, carried = lax.fori_loop(1, sp_count, turn, (output, carried))
    attn_out = output.reshape(row_count, head_count * HEAD_DIM).astype(jnp.bfloat16)
    w_pool_cols, w_attn_cols = (
        lax.all_gather(w_out_pool, "fs", axis=1, tiled=True),
        lax.all_gather(w_out_attn, "fs", axis=1, tiled=True),
    )
    pool_f = pool_out.astype(jnp.float32)
    attn_f = attn_out.astype(jnp.float32)
    pool_sq, attn_sq = lax.psum(
        (jnp.sum(pool_f * pool_f, axis=-1), jnp.sum(attn_f * attn_f, axis=-1)), "tp"
    )
    pool_normed = branch_norm(pool_out, pool_sq, POOL, pool_gain)
    attn_normed = branch_norm(attn_out, attn_sq, HEADS * HEAD_DIM, attn_gain)
    mixed = lax.psum_scatter(
        (
            jnp.dot(pool_normed, w_pool_cols, preferred_element_type=jnp.float32)
            + jnp.dot(attn_normed, w_attn_cols, preferred_element_type=jnp.float32)
        ).astype(jnp.bfloat16),
        "tp",
        scatter_dimension=0,
        tiled=True,
    )
    return mixed[None]


F32 = jnp.float32
BF = jnp.bfloat16
HALO = 16


def fused_kernel(
    tok, ng, wp, wq, wk, wv, qg, kg, off, mix, psc, pgain, again, wop, woa,
    out,
    tokf, normed, gk, gv, gq, gp, gop, goa,
    qloc, kloc, vloc, qb, kb, vb, oloc, ob,
    pin, halo, pooled, sqs, act, snd, rcv,
    lsem, wss, wrs, ass, ars, oss, ors, fss, frs, mss, mrs,
):
    sp_n = lax.axis_size("sp")
    fs_n = lax.axis_size("fs")
    me_sp, me_fs, me_tp = lax.axis_index("sp"), lax.axis_index("fs"), lax.axis_index("tp")
    near_x = me_fs + 1 - 2 * (me_fs % 2)
    near_y = (me_fs + 2) % fs_n
    other = 1 - me_tp
    rows, half_d = tok.shape
    qblk = qb.shape[1]
    lane = lax.broadcasted_iota(jnp.int32, (1, 2 * HEAD_DIM), 1)
    first = lane < HEAD_DIM

    items = ((wk, gk), (wv, gv), (wq, gq), (wp, gp), (wop, gop), (woa, goa))
    local = [pltpu.make_async_copy(src, g.at[me_fs], lsem.at[i]) for i, (src, g) in enumerate(items)]
    tok_local = pltpu.make_async_copy(tok, tokf.at[me_tp], lsem.at[6])
    tok_local.start()
    for copy in local:
        copy.start()

    barrier = pltpu.get_barrier_semaphore()
    greet = [{"fs": near_x}, {"fs": near_y}, {"tp": other}]
    greet += [{"sp": (me_sp + d) % sp_n} for d in range(1, sp_n)]
    for target in greet:
        pl.semaphore_signal(barrier, inc=1, device_id=target, device_id_type=pl.DeviceIdType.MESH)
    pl.semaphore_wait(barrier, len(greet))

    def remote(src, dst, send, recv, target):
        return pltpu.make_async_remote_copy(
            src_ref=src, dst_ref=dst, send_sem=send, recv_sem=recv,
            device_id=target, device_id_type=pl.DeviceIdType.MESH,
        )

    tok_copy = remote(tokf.at[me_tp], tokf.at[me_tp], mss.at[0], mrs.at[0], {"tp": other})
    tok_local.wait()
    tok_copy.start()

    def weight_copies(i):
        g = items[i][1]
        half = g.shape[1] // 2
        lower, upper = pl.ds(0, half), pl.ds(half, half)
        own_x = remote(g.at[me_fs], g.at[me_fs], wss.at[i, 0], wrs.at[i, 0], {"fs": near_x})
        own_y = remote(g.at[me_fs], g.at[me_fs], wss.at[i, 1], wrs.at[i, 1], {"fs": near_y})
        pass_y = remote(
            g.at[near_x, lower], g.at[near_x, lower], wss.at[i, 2], wrs.at[i, 2], {"fs": near_y}
        )
        pass_x = remote(
            g.at[near_y, upper], g.at[near_y, upper], wss.at[i, 3], wrs.at[i, 3], {"fs": near_x}
        )
        return own_x, own_y, pass_y, pass_x

    copies = [weight_copies(i) for i in range(len(items))]

    def send_own(i):
        local[i].wait()
        copies[i][0].start()
        copies[i][1].start()

    def pass_on(i):
        copies[i][0].wait_recv()
        copies[i][2].start()
        copies[i][1].wait_recv()
        copies[i][3].start()

    def arrived(i):
        copies[i][2].wait_recv()
        copies[i][3].wait_recv()

    send_own(0)
    send_own(1)

    tok_copy.wait_recv()
    chunk = 128
    width = normed.shape[2]

    def norm_rows(c, carry):
        at = pl.ds(pl.multiple_of(c * chunk, chunk), chunk)
        parts = [tokf[t, at, :].astype(F32) for t in range(2)]
        total = sum(jnp.sum(p * p, axis=-1, keepdims=True) for p in parts)
        factor = lax.rsqrt(total / (2 * half_d) + EPS)
        for f in range(fs_n):
            t, begin = divmod(f * width, half_d)
            piece = parts[t][:, begin : begin + width]
            gain = ng[:, f * width : (f + 1) * width]
            normed[f, at, :] = (piece * factor * gain).astype(BF)
        return carry

    lax.fori_loop(0, rows // chunk, norm_rows, 0)

    def project(g, finish):
        def body(r, carry):
            at = pl.ds(pl.multiple_of(r * qblk, qblk), qblk)
            acc = jnp.dot(normed[0, at, :], g[0], preferred_element_type=F32)
            for f in range(1, fs_n):
                acc = acc + jnp.dot(normed[f, at, :], g[f], preferred_element_type=F32)
            finish(r, acc)
            return carry

        lax.fori_loop(0, rows // qblk, body, 0)

    blocks = rows // qblk

    def to_heads(dest, gain, scale):
        def finish(r, acc):
            for j in range(sp_n):
                x = acc[:, j * 2 * HEAD_DIM : (j + 1) * 2 * HEAD_DIM]
                if gain is not None:
                    sq = x * x
                    low = jnp.sum(jnp.where(first, sq, 0.0), axis=-1, keepdims=True)
                    high = jnp.sum(jnp.where(first, 0.0, sq), axis=-1, keepdims=True)
                    mean = jnp.where(first, low, high) / HEAD_DIM
                    x = x * lax.rsqrt(mean + EPS) * gain[...]
                y = x.astype(BF)
                if scale is not None:
                    y = y * jnp.asarray(scale, BF)
                dest[j * blocks + r] = y

        return finish

    def exchange(i, src, dst):
        mine = pl.ds(me_sp * blocks, blocks)
        keep = pltpu.make_async_copy(src.at[mine], dst.at[mine], lsem.at[7 + i])
        sends = []
        for d in range(1, sp_n):
            peer = (me_sp + d) % sp_n
            sends.append(
                remote(
                    src.at[pl.ds(peer * blocks, blocks)], dst.at[mine],
                    ass.at[i, d - 1], ars.at[i, d - 1], {"sp": peer},
                )
            )
        return keep, sends

    swaps = [exchange(0, kloc, kb), exchange(1, vloc, vb), exchange(2, qloc, qb)]

    def start_swap(i):
        swaps[i][0].start()
        for copy in swaps[i][1]:
            copy.start()

    pass_on(0)
    pass_on(1)
    send_own(2)
    arrived(0)
    project(gk, to_heads(kloc, kg, None))
    start_swap(0)
    arrived(1)
    project(gv, to_heads(vloc, None, None))
    start_swap(1)
    pass_on(2)
    send_own(3)
    arrived(2)
    project(gq, to_heads(qloc, qg, 1.0 / math.sqrt(HEAD_DIM)))
    start_swap(2)
    pass_on(3)
    send_own(4)
    send_own(5)
    arrived(3)

    def keep_pool(r, acc):
        pin[pl.ds(pl.multiple_of(r * qblk, qblk), qblk), :] = acc.astype(BF)

    project(gp, keep_pool)
    halo_copy = remote(
        pin.at[pl.ds(rows - HALO, HALO)], halo, mss.at[1], mrs.at[1], {"sp": (me_sp + 1) % sp_n}
    )
    halo_copy.start()
    halo_copy.wait_recv()
    before = jnp.where(me_sp > 0, halo[...].astype(F32), 0.0)
    position = me_sp * rows + lax.broadcasted_iota(jnp.int32, (rows, 1), 0)
    pool_sq = jnp.zeros((rows, 1), F32)
    group_ch = mix.shape[1]
    for grp in range(mix.shape[0]):
        cols = slice(grp * group_ch, (grp + 1) * group_ch)
        ext = jnp.concatenate([before[:, cols], pin[:, cols].astype(F32)], axis=0)
        group_id = me_tp * mix.shape[0] + grp
        summed = ext
        picked = jnp.zeros_like(ext)
        for level in range(POOL_GROUPS):
            summed = summed + pltpu.roll(summed, 1 << level, 0)
            picked = jnp.where(group_id == level, summed, picked)
        window = jnp.where(group_id == 0, 2, jnp.where(group_id == 1, 4, jnp.where(group_id == 2, 8, 16)))
        counted = jnp.minimum(position + 1, window).astype(F32)
        centered = (picked[HALO:] / counted - ext[HALO:]).astype(BF)
        mixed = jnp.dot(centered, mix[grp], preferred_element_type=F32) * psc[:, cols]
        kept = mixed.astype(BF)
        pooled[:, cols] = kept
        kept_f = kept.astype(F32)
        pool_sq = pool_sq + jnp.sum(kept_f * kept_f, axis=-1, keepdims=True)
    sqs[0] = jnp.where(first, pool_sq, 0.0)

    for keep, sends in swaps:
        keep.wait()
        for copy in sends:
            copy.wait_recv()

    key_id = lax.broadcasted_iota(jnp.int32, (qblk, qblk), 0)
    col_id = lax.broadcasted_iota(jnp.int32, (qblk, qblk), 1)
    after = (key_id > col_id).astype(F32).astype(BF)
    offsets = [off[2 * me_sp + h] for h in range(2)]

    def attend(qi):
        query = qb[qi]
        zero = jnp.zeros_like(query)
        queries = (jnp.where(first, query, zero), jnp.where(first, zero, query))

        def block(kj, state, masked):
            key, val = kb[kj], vb[kj]
            result = []
            for h in range(2):
                acc, carry = state[2 * h], state[2 * h + 1]
                z = lax.dot_general(
                    queries[h], key, (((1,), (1,)), ((), ())), preferred_element_type=F32
                ) + offsets[h]
                soft = jnp.log(1.0 + jnp.exp(z))
                log_own = z - soft
                if masked:
                    soft = jnp.where(col_id < key_id, soft, 0.0)
                later = jnp.dot(soft.astype(BF), after, preferred_element_type=F32)
                weight = jnp.exp(log_own - later - carry)
                if masked:
                    weight = jnp.where(col_id < key_id, weight, 0.0)
                acc = acc + jnp.dot(weight.astype(BF), val, preferred_element_type=F32)
                carry = carry + later[:, :1] + soft[:, :1]
                result += [acc, carry]
            return tuple(result)

        start = (jnp.zeros((qblk, 2 * HEAD_DIM), F32), jnp.zeros((qblk, 1), F32)) * 2
        state = block(qi, start, True)
        state = lax.fori_loop(0, qi, lambda n, s: block(qi - 1 - n, s, False), state)
        oloc[qi] = jnp.where(first, state[0], state[2]).astype(BF)

    def attend_rows(d):
        place = (me_sp + d) % sp_n

        def one(r, carry):
            attend(place * blocks + r)
            return carry

        lax.fori_loop(0, blocks, one, 0)

    def give_back(d):
        place = (me_sp + d) % sp_n
        return remote(
            oloc.at[pl.ds(place * blocks, blocks)], ob.at[pl.ds(me_sp * blocks, blocks)],
            oss.at[d - 1], ors.at[d - 1], {"sp": place},
        )

    attend_rows(1)
    give_back(1).start()
    pass_on(4)
    pass_on(5)

    def middle(d, carry):
        attend_rows(d)
        give_back(d).start()
        return carry

    lax.fori_loop(2, sp_n, middle, 0)
    attend_rows(sp_n)
    mine = pl.ds(me_sp * blocks, blocks)
    keep_out = pltpu.make_async_copy(oloc.at[mine], ob.at[mine], lsem.at[10])
    keep_out.start()
    keep_out.wait()
    for d in range(1, sp_n):
        give_back(d).wait_recv()

    attn_sq = jnp.zeros((rows, 1), F32)
    attended = [ob[j * blocks : (j + 1) * blocks].reshape(rows, 2 * HEAD_DIM).astype(F32) for j in range(sp_n)]
    for piece in attended:
        attn_sq = attn_sq + jnp.sum(piece * piece, axis=-1, keepdims=True)
    sqs[0] = jnp.where(first, sqs[0], attn_sq)
    sq_copy = remote(sqs.at[0], sqs.at[1], mss.at[2], mrs.at[2], {"tp": other})
    sq_copy.start()
    arrived(4)
    arrived(5)
    sq_copy.wait_recv()
    totals = sqs[0] + sqs[1]
    pool_ch = pooled.shape[1]
    attn_ch = goa.shape[1]
    pool_factor = lax.rsqrt(totals[:, :1] / (2 * pool_ch) + EPS)
    attn_factor = lax.rsqrt(totals[:, HEAD_DIM : HEAD_DIM + 1] / (2 * attn_ch) + EPS)
    act[:, :pool_ch] = (pooled[...].astype(F32) * pool_factor * pgain[...]).astype(BF)
    for j in range(sp_n):
        cols = slice(j * 2 * HEAD_DIM, (j + 1) * 2 * HEAD_DIM)
        spot = slice(pool_ch + j * 2 * HEAD_DIM, pool_ch + (j + 1) * 2 * HEAD_DIM)
        piece = ob[j * blocks : (j + 1) * blocks].reshape(rows, 2 * HEAD_DIM).astype(F32)
        act[:, spot] = (piece * attn_factor * again[:, cols]).astype(BF)

    share = rows // 2

    def partial_sum(which, f):
        at = pl.ds(pl.multiple_of(which * share, share), share)
        return jnp.dot(act[at, :pool_ch], gop[f], preferred_element_type=F32) + jnp.dot(
            act[at, pool_ch:], goa[f], preferred_element_type=F32
        )

    def hand_over(f):
        return remote(snd.at[f], rcv.at[f], fss.at[f], frs.at[f], {"tp": other})

    def theirs(f, carry):
        snd[f] = partial_sum(other, f).astype(BF)
        hand_over(f).start()
        return carry

    lax.fori_loop(0, fs_n, theirs, 0)
    out_w = gop.shape[2]

    def ours(f, carry):
        total = partial_sum(me_tp, f)
        hand_over(f).wait_recv()
        total = total + rcv[f].astype(F32)
        out[:, pl.ds(pl.multiple_of(f * out_w, out_w), out_w)] = total.astype(BF)
        return carry

    lax.fori_loop(0, fs_n, ours, 0)

    tok_copy.wait_send()
    halo_copy.wait_send()
    sq_copy.wait_send()
    for group in copies:
        for copy in group:
            copy.wait_send()
    for _, sends in swaps:
        for copy in sends:
            copy.wait_send()
    for d in range(1, sp_n):
        give_back(d).wait_send()
    for f in range(fs_n):
        hand_over(f).wait_send()


def fused_shards(
    tokens, norm_gain, w_pool_in, w_query, w_key, w_value, query_gain, key_gain,
    stick_offset, pool_mix, pool_scale, pool_gain, attn_gain, w_out_pool, w_out_attn,
):
    sp_n, fs_n = lax.axis_size("sp"), lax.axis_size("fs")
    _, rows, half_d = tokens.shape
    depth, attn_ch = w_query.shape
    pool_ch = w_pool_in.shape[1]
    out_w = w_out_pool.shape[1]
    qblk = rows // 2
    pair = 2 * HEAD_DIM
    nblk = sp_n * (rows // qblk)
    vmem = pl.BlockSpec(memory_space=pltpu.VMEM)
    hbm = pl.BlockSpec(memory_space=pl.ANY)
    smem = pl.BlockSpec(memory_space=pltpu.SMEM)
    dma = pltpu.SemaphoreType.DMA
    heads = pltpu.VMEM((nblk, qblk, pair), BF)
    result = pl.pallas_call(
        fused_kernel,
        out_shape=jax.ShapeDtypeStruct((rows // 2, fs_n * out_w), BF),
        in_specs=[hbm, vmem, hbm, hbm, hbm, hbm, vmem, vmem, smem, vmem, vmem, vmem, vmem, hbm, hbm],
        out_specs=vmem,
        scratch_shapes=[
            pltpu.VMEM((2, rows, half_d), BF),
            pltpu.VMEM((fs_n, rows, depth), BF),
            pltpu.VMEM((fs_n, depth, attn_ch), BF),
            pltpu.VMEM((fs_n, depth, attn_ch), BF),
            pltpu.VMEM((fs_n, depth, attn_ch), BF),
            pltpu.VMEM((fs_n, depth, pool_ch), BF),
            pltpu.VMEM((fs_n, pool_ch, out_w), BF),
            pltpu.VMEM((fs_n, attn_ch, out_w), BF),
            heads, heads, heads, heads, heads, heads, heads, heads,
            pltpu.VMEM((rows, pool_ch), BF),
            pltpu.VMEM((HALO, pool_ch), BF),
            pltpu.VMEM((rows, pool_ch), BF),
            pltpu.VMEM((2, rows, pair), F32),
            pltpu.VMEM((rows, pool_ch + attn_ch), BF),
            pltpu.VMEM((fs_n, rows // 2, out_w), BF),
            pltpu.VMEM((fs_n, rows // 2, out_w), BF),
            dma((11,)), dma((6, 4)), dma((6, 4)), dma((3, sp_n - 1)), dma((3, sp_n - 1)),
            dma((sp_n - 1,)), dma((sp_n - 1,)), dma((fs_n,)), dma((fs_n,)), dma((3,)), dma((3,)),
        ],
        compiler_params=pltpu.CompilerParams(
            collective_id=0, has_side_effects=True, vmem_limit_bytes=60 * 1024 * 1024
        ),
        name="mixer",
    )(
        tokens[0], norm_gain[None], w_pool_in, w_query, w_key, w_value,
        jnp.tile(query_gain, 2)[None], jnp.tile(key_gain, 2)[None], stick_offset, pool_mix,
        pool_scale[None], pool_gain.astype(F32)[None], attn_gain.astype(F32)[None],
        w_out_pool, w_out_attn,
    )
    return result[None]


def suits_fused(mesh):
    shape = mesh.shape
    return shape["tp"] == 2 and shape["fs"] == 4 and HEADS // shape["tp"] == 2 * shape["sp"]


def solution(mesh):
    in_specs = (
        P("fs", "sp", "tp"),
        P(),
        P("fs", "tp"),
        P("fs", "tp"),
        P("fs", "tp"),
        P("fs", "tp"),
        P(),
        P(),
        P("tp"),
        P("tp", None, None),
        P("tp"),
        P("tp"),
        P("tp"),
        P("tp", "fs"),
        P("tp", "fs"),
    )
    out_specs = P("fs", ("sp", "tp"), None)
    body = fused_shards if suits_fused(mesh) else shards
    return jax.shard_map(body, mesh=mesh, in_specs=in_specs, out_specs=out_specs, check_vma=False)
```

```python
import math

import jax
import jax.numpy as jnp
from jax import lax
from jax.experimental import pallas as pl
from jax.experimental.pallas import tpu as pltpu
from jax.sharding import PartitionSpec as P

HEADS = 16
HEAD_DIM = 64
POOL = 512
POOL_GROUPS = 4


EPS = 1e-06


def shifted_2(value, axis, steps):
    count = lax.axis_size(axis)
    initial, last = (max(0, -steps), min(count, count - steps))
    return lax.ppermute(value, axis, [(source, source + steps) for source in range(initial, last)])


def head_norm(projected, gain, head_count):
    split = projected.reshape(projected.shape[0], head_count, HEAD_DIM)
    factor = lax.rsqrt(jnp.mean(split * split, axis=-1, keepdims=True) + EPS)
    return (split * factor * gain).astype(jnp.bfloat16)


def stick_block(query, key_heads, value_heads, offset, carried, row_offset, score_scale):
    scores = (
        jnp.einsum("thd,khd->htk", query, key_heads, preferred_element_type=jnp.float32)
        * score_scale
        + offset[:, None, None]
    )
    keep = jax.nn.log_sigmoid(-scores)
    if row_offset is not None:
        shape = (query.shape[0], key_heads.shape[0])
        earlier = (
            lax.broadcasted_iota(jnp.int32, shape, 1)
            < lax.broadcasted_iota(jnp.int32, shape, 0) + row_offset
        )
        keep = jnp.where(earlier[None], keep, 0.0)
    running = jnp.cumsum(keep, axis=2)
    block_total = running[:, :, -1]
    log_weight = (
        jax.nn.log_sigmoid(scores) + block_total[:, :, None] - running + carried[:, :, None]
    )
    weight = jnp.exp(log_weight)
    if row_offset is not None:
        weight = jnp.where(earlier[None], weight, 0.0)
    weight = weight.astype(jnp.bfloat16)
    block_out = jnp.einsum("htk,khd->thd", weight, value_heads, preferred_element_type=jnp.float32)
    return (block_out, block_total)


def branch_norm(values_in, squares, width, gain):
    values_f = values_in.astype(jnp.float32)
    factor = lax.rsqrt(squares / width + EPS)
    return (values_f * factor[:, None] * gain.astype(jnp.float32)).astype(jnp.bfloat16)


def shards(
    tokens,
    norm_gain,
    w_pool_in,
    w_query,
    w_key,
    w_value,
    query_gain,
    key_gain,
    stick_offset,
    pool_mix,
    pool_scale,
    pool_gain,
    attn_gain,
    w_out_pool,
    w_out_attn,
):
    whole = lax.all_gather(tokens, "tp", axis=2, tiled=True)[0]
    whole_f = whole.astype(jnp.float32)
    normed = (
        whole_f * lax.rsqrt(jnp.mean(whole_f * whole_f, axis=-1, keepdims=True) + EPS) * norm_gain
    ).astype(jnp.bfloat16)
    row_count = normed.shape[0]
    pieces = (
        lax.all_gather(w_pool_in, "fs", axis=0, tiled=True),
        lax.all_gather(w_query, "fs", axis=0, tiled=True),
        lax.all_gather(w_key, "fs", axis=0, tiled=True),
        lax.all_gather(w_value, "fs", axis=0, tiled=True),
    )
    pool_raw, query_raw, key_raw, value_raw = tuple(
        (jnp.dot(normed, piece, preferred_element_type=jnp.float32) for piece in pieces)
    )
    head_count = query_raw.shape[1] // HEAD_DIM
    query = head_norm(query_raw, query_gain, head_count)
    key_heads = head_norm(key_raw, key_gain, head_count)
    value_heads = value_raw.astype(jnp.bfloat16).reshape(row_count, head_count, HEAD_DIM)
    reach = 16
    pool_in = pool_raw.astype(jnp.bfloat16)
    previous = shifted_2(pool_in[row_count - reach :], "sp", 1)
    extended = jnp.concatenate([previous, pool_in], axis=0).astype(jnp.float32)
    pool_cols = pool_in.shape[1]
    group_ch = POOL // POOL_GROUPS
    local_groups = pool_cols // group_ch
    group_ids = (
        lax.axis_index("tp") * local_groups + jnp.arange(pool_cols, dtype=jnp.int32) // group_ch
    )
    window = jnp.left_shift(jnp.int32(2), group_ids)
    summed = jnp.zeros((row_count, pool_cols), jnp.float32)
    for behind in range(reach):
        shifted = extended[reach - behind : reach - behind + row_count]
        summed = summed + jnp.where(behind < window[None, :], shifted, 0.0)
    sp_index = lax.axis_index("sp")
    position = sp_index * row_count + jnp.arange(row_count, dtype=jnp.int32)
    counted = jnp.minimum(position[:, None] + 1, window[None, :]).astype(jnp.float32)
    centered = (summed / counted - extended[reach:]).astype(jnp.bfloat16)
    pooled = jnp.einsum(
        "tgc,gcd->tgd",
        centered.reshape(row_count, local_groups, group_ch),
        pool_mix,
        preferred_element_type=jnp.float32,
    )
    pool_out = (pooled.reshape(row_count, pool_cols) * pool_scale).astype(jnp.bfloat16)
    score_scale = 1.0 / math.sqrt(HEAD_DIM)
    sp_count = lax.axis_size("sp")
    key_value = jnp.stack([key_heads, value_heads])
    start_carry = jnp.zeros((head_count, row_count), jnp.float32)
    output, carried = stick_block(
        query, key_heads, value_heads, stick_offset, start_carry, 0, score_scale
    )
    everything = lax.all_gather(key_value, "sp", axis=1, tiled=True)

    def turn(turn_index, state):
        acc_out, acc_carry = state
        source = jnp.maximum(sp_index - turn_index, 0)
        block = lax.dynamic_slice_in_dim(everything, source * row_count, row_count, 1)
        block_out, block_total = stick_block(
            query, block[0], block[1], stick_offset, acc_carry, None, score_scale
        )
        usable = turn_index <= sp_index
        return (
            acc_out + jnp.where(usable, block_out, 0.0),
            acc_carry + jnp.where(usable, block_total, 0.0),
        )

    output, carried = lax.fori_loop(1, sp_count, turn, (output, carried))
    attn_out = output.reshape(row_count, head_count * HEAD_DIM).astype(jnp.bfloat16)
    w_pool_cols, w_attn_cols = (
        lax.all_gather(w_out_pool, "fs", axis=1, tiled=True),
        lax.all_gather(w_out_attn, "fs", axis=1, tiled=True),
    )
    pool_f = pool_out.astype(jnp.float32)
    attn_f = attn_out.astype(jnp.float32)
    pool_sq, attn_sq = lax.psum(
        (jnp.sum(pool_f * pool_f, axis=-1), jnp.sum(attn_f * attn_f, axis=-1)), "tp"
    )
    pool_normed = branch_norm(pool_out, pool_sq, POOL, pool_gain)
    attn_normed = branch_norm(attn_out, attn_sq, HEADS * HEAD_DIM, attn_gain)
    mixed = lax.psum_scatter(
        (
            jnp.dot(pool_normed, w_pool_cols, preferred_element_type=jnp.float32)
            + jnp.dot(attn_normed, w_attn_cols, preferred_element_type=jnp.float32)
        ).astype(jnp.bfloat16),
        "tp",
        scatter_dimension=0,
        tiled=True,
    )
    return mixed[None]


F32 = jnp.float32
BF = jnp.bfloat16
HALO = 16


def fused_kernel(
    tok, ng, wp, wq, wk, wv, qg, kg, off, mix, psc, pgain, again, wop, woa,
    out,
    tokf, normed, gk, gv, gq, gp, gop, goa,
    qloc, kloc, vloc, qb, kb, vb, oloc, ob,
    pin, halo, pooled, sqs, act, snd, rcv,
    lsem, wss, wrs, ass, ars, oss, ors, fss, frs, mss, mrs,
):
    sp_n = lax.axis_size("sp")
    fs_n = lax.axis_size("fs")
    me_sp, me_fs, me_tp = lax.axis_index("sp"), lax.axis_index("fs"), lax.axis_index("tp")
    near_x = me_fs + 1 - 2 * (me_fs % 2)
    near_y = (me_fs + 2) % fs_n
    other = 1 - me_tp
    rows, half_d = tok.shape
    qblk = qb.shape[1]
    lane = lax.broadcasted_iota(jnp.int32, (1, 2 * HEAD_DIM), 1)
    first = lane < HEAD_DIM

    def row(ref, begin, size):
        return ref[begin : begin + size].astype(F32)[None, :]

    def twice(ref):
        single = row(ref, 0, HEAD_DIM)
        return jnp.concatenate([single, single], axis=1)


    items = ((wk, gk), (wv, gv), (wq, gq), (wp, gp), (wop, gop), (woa, goa))
    local = [pltpu.make_async_copy(src, g.at[me_fs], lsem.at[i]) for i, (src, g) in enumerate(items)]
    tok_local = pltpu.make_async_copy(tok, tokf.at[me_tp], lsem.at[6])
    tok_local.start()
    for copy in local:
        copy.start()

    barrier = pltpu.get_barrier_semaphore()
    greet = [{"fs": near_x}, {"fs": near_y}, {"tp": other}]
    greet += [{"sp": (me_sp + d) % sp_n} for d in range(1, sp_n)]
    for target in greet:
        pl.semaphore_signal(barrier, inc=1, device_id=target, device_id_type=pl.DeviceIdType.MESH)
    pl.semaphore_wait(barrier, len(greet))

    def remote(src, dst, send, recv, target):
        return pltpu.make_async_remote_copy(
            src_ref=src, dst_ref=dst, send_sem=send, recv_sem=recv,
            device_id=target, device_id_type=pl.DeviceIdType.MESH,
        )

    tok_copy = remote(tokf.at[me_tp], tokf.at[me_tp], mss.at[0], mrs.at[0], {"tp": other})
    tok_local.wait()
    tok_copy.start()

    def weight_copies(i):
        g = items[i][1]
        half = g.shape[1] // 2
        lower, upper = pl.ds(0, half), pl.ds(half, half)
        own_x = remote(g.at[me_fs], g.at[me_fs], wss.at[i, 0], wrs.at[i, 0], {"fs": near_x})
        own_y = remote(g.at[me_fs], g.at[me_fs], wss.at[i, 1], wrs.at[i, 1], {"fs": near_y})
        pass_y = remote(
            g.at[near_x, lower], g.at[near_x, lower], wss.at[i, 2], wrs.at[i, 2], {"fs": near_y}
        )
        pass_x = remote(
            g.at[near_y, upper], g.at[near_y, upper], wss.at[i, 3], wrs.at[i, 3], {"fs": near_x}
        )
        return own_x, own_y, pass_y, pass_x

    plane = me_sp % 2
    full_peer = me_fs + (1 - plane) * (near_x - me_fs) + plane * (near_y - me_fs)
    half_peer = me_fs + (1 - plane) * (near_y - me_fs) + plane * (near_x - me_fs)
    diagonal = fs_n - 1 - me_fs
    twin = me_sp + 1 - 2 * plane

    def traded_copies(i):
        g = items[i][1]
        half = g.shape[1] // 2
        here = pl.ds(pl.multiple_of(plane * half, half), half)
        there = pl.ds(pl.multiple_of((1 - plane) * half, half), half)
        plan = (
            (me_fs, here, {"fs": full_peer}),
            (me_fs, there, {"fs": full_peer}),
            (me_fs, here, {"fs": half_peer}),
            (full_peer, here, {"fs": half_peer}),
            (full_peer, here, {"sp": twin}),
            (diagonal, here, {"sp": twin}),
        )
        return [
            remote(g.at[b, r], g.at[b, r], wss.at[i, n], wrs.at[i, n], target)
            for n, (b, r, target) in enumerate(plan)
        ]

    traded = (0, 1, 5)
    copies = [
        traded_copies(i) if i in traded else weight_copies(i) for i in range(len(items))
    ]

    def trade_relay(i):
        copies[i][0].wait_recv()
        copies[i][3].start()
        copies[i][4].start()

    def trade_last(i):
        copies[i][3].wait_recv()
        copies[i][5].start()

    def trade_done(i):
        for n in (1, 2, 4, 5):
            copies[i][n].wait_recv()

    def send_own(i):
        local[i].wait()
        copies[i][0].start()
        copies[i][1].start()

    def pass_on(i):
        copies[i][0].wait_recv()
        copies[i][2].start()
        copies[i][1].wait_recv()
        copies[i][3].start()

    def arrived(i):
        copies[i][2].wait_recv()
        copies[i][3].wait_recv()

    local[0].wait()
    for n in (0, 2, 1):
        copies[0][n].start()
    local[1].wait()
    for n in (0, 1):
        copies[1][n].start()

    tok_copy.wait_recv()
    chunk = 128
    width = normed.shape[2]

    def norm_rows(c, carry):
        at = pl.ds(pl.multiple_of(c * chunk, chunk), chunk)
        parts = [tokf[t, at, :].astype(F32) for t in range(2)]
        total = sum(jnp.sum(p * p, axis=-1, keepdims=True) for p in parts)
        factor = lax.rsqrt(total / (2 * half_d) + EPS)
        for f in range(fs_n):
            t, begin = divmod(f * width, half_d)
            piece = parts[t][:, begin : begin + width]
            gain = row(ng, f * width, width)
            normed[f, at, :] = (piece * factor * gain).astype(BF)
        return carry

    lax.fori_loop(0, rows // chunk, norm_rows, 0)

    def project(g, finish):
        def body(r, carry):
            at = pl.ds(pl.multiple_of(r * qblk, qblk), qblk)
            acc = jnp.dot(normed[0, at, :], g[0], preferred_element_type=F32)
            for f in range(1, fs_n):
                acc = acc + jnp.dot(normed[f, at, :], g[f], preferred_element_type=F32)
            finish(r, acc)
            return carry

        lax.fori_loop(0, rows // qblk, body, 0)

    blocks = rows // qblk

    def to_heads(dest, gain, scale):
        def finish(r, acc):
            for j in range(sp_n):
                x = acc[:, j * 2 * HEAD_DIM : (j + 1) * 2 * HEAD_DIM]
                if gain is not None:
                    sq = x * x
                    low = jnp.sum(jnp.where(first, sq, 0.0), axis=-1, keepdims=True)
                    high = jnp.sum(jnp.where(first, 0.0, sq), axis=-1, keepdims=True)
                    mean = jnp.where(first, low, high) / HEAD_DIM
                    x = x * lax.rsqrt(mean + EPS) * gain
                y = x.astype(BF)
                if scale is not None:
                    y = y * jnp.asarray(scale, BF)
                dest[j * blocks + r] = y

        return finish

    def exchange(i, src, dst):
        mine = pl.ds(me_sp * blocks, blocks)
        keep = pltpu.make_async_copy(src.at[mine], dst.at[mine], lsem.at[7 + i])
        sends = []
        for d in range(1, sp_n):
            peer = (me_sp + d) % sp_n
            sends.append(
                remote(
                    src.at[pl.ds(peer * blocks, blocks)], dst.at[mine],
                    ass.at[i, d - 1], ars.at[i, d - 1], {"sp": peer},
                )
            )
        return keep, sends

    swaps = [exchange(0, kloc, kb), exchange(1, vloc, vb), exchange(2, qloc, qb)]

    def start_swap(i):
        swaps[i][0].start()
        for copy in swaps[i][1]:
            copy.start()

    trade_relay(0)
    copies[1][2].start()
    trade_last(0)
    trade_relay(1)
    send_own(2)
    trade_done(0)
    project(gk, to_heads(kloc, twice(kg), None))
    start_swap(0)
    trade_last(1)
    trade_done(1)
    project(gv, to_heads(vloc, None, None))
    start_swap(1)
    pass_on(2)
    send_own(3)
    arrived(2)
    project(gq, to_heads(qloc, twice(qg), 1.0 / math.sqrt(HEAD_DIM)))
    start_swap(2)
    pass_on(3)
    send_own(4)
    local[5].wait()
    for n in (0, 2, 1):
        copies[5][n].start()
    arrived(3)

    def keep_pool(r, acc):
        pin[pl.ds(pl.multiple_of(r * qblk, qblk), qblk), :] = acc.astype(BF)

    project(gp, keep_pool)
    halo_copy = remote(
        pin.at[pl.ds(rows - HALO, HALO)], halo, mss.at[1], mrs.at[1], {"sp": (me_sp + 1) % sp_n}
    )
    halo_copy.start()
    halo_copy.wait_recv()
    before = jnp.where(me_sp > 0, halo[...].astype(F32), 0.0)
    position = me_sp * rows + lax.broadcasted_iota(jnp.int32, (rows, 1), 0)
    pool_sq = jnp.zeros((rows, 1), F32)
    group_ch = mix.shape[1]
    for grp in range(mix.shape[0]):
        cols = slice(grp * group_ch, (grp + 1) * group_ch)
        ext = jnp.concatenate([before[:, cols], pin[:, cols].astype(F32)], axis=0)
        group_id = me_tp * mix.shape[0] + grp
        summed = ext
        picked = jnp.zeros_like(ext)
        for level in range(POOL_GROUPS):
            summed = summed + pltpu.roll(summed, 1 << level, 0)
            picked = jnp.where(group_id == level, summed, picked)
        window = jnp.where(group_id == 0, 2, jnp.where(group_id == 1, 4, jnp.where(group_id == 2, 8, 16)))
        counted = jnp.minimum(position + 1, window).astype(F32)
        centered = (picked[HALO:] / counted - ext[HALO:]).astype(BF)
        mixed = jnp.dot(centered, mix[grp], preferred_element_type=F32) * row(psc, grp * group_ch, group_ch)
        kept = mixed.astype(BF)
        pooled[:, cols] = kept
        kept_f = kept.astype(F32)
        pool_sq = pool_sq + jnp.sum(kept_f * kept_f, axis=-1, keepdims=True)
    sqs[0] = jnp.where(first, pool_sq, 0.0)

    for keep, sends in swaps:
        keep.wait()
        for copy in sends:
            copy.wait_recv()

    key_id = lax.broadcasted_iota(jnp.int32, (qblk, qblk), 0)
    col_id = lax.broadcasted_iota(jnp.int32, (qblk, qblk), 1)
    after = (key_id > col_id).astype(F32).astype(BF)
    offsets = [off[2 * me_sp + h] for h in range(2)]

    def attend(qi):
        query = qb[qi]
        zero = jnp.zeros_like(query)
        queries = (jnp.where(first, query, zero), jnp.where(first, zero, query))

        def block(kj, state, masked):
            key, val = kb[kj], vb[kj]
            result = []
            for h in range(2):
                acc, carry = state[2 * h], state[2 * h + 1]
                z = lax.dot_general(
                    queries[h], key, (((1,), (1,)), ((), ())), preferred_element_type=F32
                ) + offsets[h]
                soft = jnp.log(1.0 + jnp.exp(z))
                log_own = z - soft
                if masked:
                    soft = jnp.where(col_id < key_id, soft, 0.0)
                later = jnp.dot(soft.astype(BF), after, preferred_element_type=F32)
                weight = jnp.exp(log_own - later - carry)
                if masked:
                    weight = jnp.where(col_id < key_id, weight, 0.0)
                acc = acc + jnp.dot(weight.astype(BF), val, preferred_element_type=F32)
                carry = carry + later[:, :1] + soft[:, :1]
                result += [acc, carry]
            return tuple(result)

        start = (jnp.zeros((qblk, 2 * HEAD_DIM), F32), jnp.zeros((qblk, 1), F32)) * 2
        state = block(qi, start, True)
        state = lax.fori_loop(0, qi, lambda n, s: block(qi - 1 - n, s, False), state)
        oloc[qi] = jnp.where(first, state[0], state[2]).astype(BF)

    def attend_rows(d):
        place = (me_sp + d) % sp_n

        def one(r, carry):
            attend(place * blocks + r)
            return carry

        lax.fori_loop(0, blocks, one, 0)

    def give_back(d):
        place = (me_sp + d) % sp_n
        return remote(
            oloc.at[pl.ds(place * blocks, blocks)], ob.at[pl.ds(me_sp * blocks, blocks)],
            oss.at[d - 1], ors.at[d - 1], {"sp": place},
        )

    pass_on(4)
    for d in range(1, sp_n):
        attend_rows(d)
        give_back(d).start()
        if d == 1:
            trade_relay(5)
        if d == 2:
            trade_last(5)
    attend_rows(sp_n)
    mine = pl.ds(me_sp * blocks, blocks)
    keep_out = pltpu.make_async_copy(oloc.at[mine], ob.at[mine], lsem.at[10])
    keep_out.start()
    keep_out.wait()
    for d in range(1, sp_n):
        give_back(d).wait_recv()

    attn_sq = jnp.zeros((rows, 1), F32)
    attended = [ob[j * blocks : (j + 1) * blocks].reshape(rows, 2 * HEAD_DIM).astype(F32) for j in range(sp_n)]
    for piece in attended:
        attn_sq = attn_sq + jnp.sum(piece * piece, axis=-1, keepdims=True)
    sqs[0] = jnp.where(first, sqs[0], attn_sq)
    sq_copy = remote(sqs.at[0], sqs.at[1], mss.at[2], mrs.at[2], {"tp": other})
    sq_copy.start()
    arrived(4)
    trade_done(5)
    sq_copy.wait_recv()
    totals = sqs[0] + sqs[1]
    pool_ch = pooled.shape[1]
    attn_ch = goa.shape[1]
    pool_factor = lax.rsqrt(totals[:, :1] / (2 * pool_ch) + EPS)
    attn_factor = lax.rsqrt(totals[:, HEAD_DIM : HEAD_DIM + 1] / (2 * attn_ch) + EPS)
    act[:, :pool_ch] = (pooled[...].astype(F32) * pool_factor * row(pgain, 0, pool_ch)).astype(BF)
    for j in range(sp_n):
        spot = slice(pool_ch + j * 2 * HEAD_DIM, pool_ch + (j + 1) * 2 * HEAD_DIM)
        piece = ob[j * blocks : (j + 1) * blocks].reshape(rows, 2 * HEAD_DIM).astype(F32)
        act[:, spot] = (piece * attn_factor * row(again, j * 2 * HEAD_DIM, 2 * HEAD_DIM)).astype(BF)

    share = rows // 2

    def partial_sum(which, f):
        at = pl.ds(pl.multiple_of(which * share, share), share)
        return jnp.dot(act[at, :pool_ch], gop[f], preferred_element_type=F32) + jnp.dot(
            act[at, pool_ch:], goa[f], preferred_element_type=F32
        )

    def hand_over(f):
        return remote(snd.at[f], rcv.at[f], fss.at[f], frs.at[f], {"tp": other})

    def theirs(f, carry):
        snd[f] = partial_sum(other, f).astype(BF)
        hand_over(f).start()
        return carry

    lax.fori_loop(0, fs_n, theirs, 0)
    out_w = gop.shape[2]

    def ours(f, carry):
        total = partial_sum(me_tp, f)
        hand_over(f).wait_recv()
        total = total + rcv[f].astype(F32)
        out[:, pl.ds(pl.multiple_of(f * out_w, out_w), out_w)] = total.astype(BF)
        return carry

    lax.fori_loop(0, fs_n, ours, 0)

    tok_copy.wait_send()
    halo_copy.wait_send()
    sq_copy.wait_send()
    for group in copies:
        for copy in group:
            copy.wait_send()
    for _, sends in swaps:
        for copy in sends:
            copy.wait_send()
    for d in range(1, sp_n):
        give_back(d).wait_send()
    for f in range(fs_n):
        hand_over(f).wait_send()


def fused_shards(
    tokens, norm_gain, w_pool_in, w_query, w_key, w_value, query_gain, key_gain,
    stick_offset, pool_mix, pool_scale, pool_gain, attn_gain, w_out_pool, w_out_attn,
):
    sp_n, fs_n = lax.axis_size("sp"), lax.axis_size("fs")
    _, rows, half_d = tokens.shape
    depth, attn_ch = w_query.shape
    pool_ch = w_pool_in.shape[1]
    out_w = w_out_pool.shape[1]
    qblk = rows // 2
    pair = 2 * HEAD_DIM
    nblk = sp_n * (rows // qblk)
    vmem = pl.BlockSpec(memory_space=pltpu.VMEM)
    hbm = pl.BlockSpec(memory_space=pl.ANY)
    smem = pl.BlockSpec(memory_space=pltpu.SMEM)
    dma = pltpu.SemaphoreType.DMA
    heads = pltpu.VMEM((nblk, qblk, pair), BF)
    result = pl.pallas_call(
        fused_kernel,
        out_shape=jax.ShapeDtypeStruct((rows // 2, fs_n * out_w), BF),
        in_specs=[hbm, vmem, hbm, hbm, hbm, hbm, vmem, vmem, smem, vmem, vmem, vmem, vmem, hbm, hbm],
        out_specs=vmem,
        scratch_shapes=[
            pltpu.VMEM((2, rows, half_d), BF),
            pltpu.VMEM((fs_n, rows, depth), BF),
            pltpu.VMEM((fs_n, depth, attn_ch), BF),
            pltpu.VMEM((fs_n, depth, attn_ch), BF),
            pltpu.VMEM((fs_n, depth, attn_ch), BF),
            pltpu.VMEM((fs_n, depth, pool_ch), BF),
            pltpu.VMEM((fs_n, pool_ch, out_w), BF),
            pltpu.VMEM((fs_n, attn_ch, out_w), BF),
            heads, heads, heads, heads, heads, heads, heads, heads,
            pltpu.VMEM((rows, pool_ch), BF),
            pltpu.VMEM((HALO, pool_ch), BF),
            pltpu.VMEM((rows, pool_ch), BF),
            pltpu.VMEM((2, rows, pair), F32),
            pltpu.VMEM((rows, pool_ch + attn_ch), BF),
            pltpu.VMEM((fs_n, rows // 2, out_w), BF),
            pltpu.VMEM((fs_n, rows // 2, out_w), BF),
            dma((11,)), dma((6, 6)), dma((6, 6)), dma((3, sp_n - 1)), dma((3, sp_n - 1)),
            dma((sp_n - 1,)), dma((sp_n - 1,)), dma((fs_n,)), dma((fs_n,)), dma((3,)), dma((3,)),
        ],
        compiler_params=pltpu.CompilerParams(
            collective_id=0, has_side_effects=True, vmem_limit_bytes=60 * 1024 * 1024
        ),
        name="mixer",
    )(
        tokens[0], norm_gain, w_pool_in, w_query, w_key, w_value, query_gain, key_gain,
        stick_offset, pool_mix, pool_scale, pool_gain, attn_gain,
        w_out_pool, w_out_attn,
    )
    return result[None]


def suits_fused(mesh):
    shape = mesh.shape
    return shape["tp"] == 2 and shape["fs"] == 4 and HEADS // shape["tp"] == 2 * shape["sp"]


def solution(mesh):
    in_specs = (
        P("fs", "sp", "tp"),
        P(),
        P("fs", "tp"),
        P("fs", "tp"),
        P("fs", "tp"),
        P("fs", "tp"),
        P(),
        P(),
        P("tp"),
        P("tp", None, None),
        P("tp"),
        P("tp"),
        P("tp"),
        P("tp", "fs"),
        P("tp", "fs"),
    )
    out_specs = P("fs", ("sp", "tp"), None)
    body = fused_shards if suits_fused(mesh) else shards
    return jax.shard_map(body, mesh=mesh, in_specs=in_specs, out_specs=out_specs, check_vma=False)
```
